32 devices in a mesh: ep: 8 (over z, y), tp: 4 (over x, core).
Axes of the slice: x: 2, y: 2, z: 4, core: 2. Of those that a mesh axis runs over, the one named last changes fastest.
Arguments:
- tokens: bfloat16 [128, 2048], P('ep', 'tp'), may hold values from -40 to 40
- kv_cache: bfloat16 [128, 1024, 512], P('ep', None, 'tp'), may hold values from -1000 to 1000
- cum_gate: float32 [128, 16, 1024], P('ep', 'tp'), may hold values from -400 to 0, as said below
- lengths: int32 [128], P('ep'), may hold values from 256 to 1024
- w_query: bfloat16 [2048, 1024], P(None, 'tp'), may hold values from -0.125 to 0.125
- w_key: bfloat16 [2048, 256], P(None, 'tp'), may hold values from -0.125 to 0.125
- w_value: bfloat16 [2048, 256], P(None, 'tp'), may hold values from -0.125 to 0.125
- w_forget: bfloat16 [2048, 16], P(None, 'tp'), may hold values from -0.5 to 0.5
- forget_bias: float32 [16], P('tp'), may hold values from -2.5 to 1.5
- w_out: bfloat16 [1024, 2048], P('tp'), may hold values from -0.1875 to 0.1875
- attn_gain: bfloat16 [2048], replicated, may hold values from 0.099609375 to 1.8984375
- ffn_gain: bfloat16 [2048], replicated, may hold values from 0.099609375 to 1.8984375
- mix_gate: bfloat16 [2048], replicated, may hold values from -0.125 to 0.125
- expert_gate: bfloat16 [8, 2048, 1024], P('ep', None, 'tp'), may hold values from -0.125 to 0.125
- expert_up: bfloat16 [8, 2048, 1024], P('ep', None, 'tp'), may hold values from -0.125 to 0.125
- expert_down: bfloat16 [8, 1024, 2048], P('ep', 'tp'), may hold values from -0.1875 to 0.1875
- chosen: int32 [128, 2], P('ep'), may hold values from 0 to 7, as said below
- route_weight: float32 [128, 2], P('ep'), may hold values from 0.5 to 1.5
- dense_gate: bfloat16 [2048, 1024], P(None, 'tp'), may hold values from -0.125 to 0.125
- dense_up: bfloat16 [2048, 1024], P(None, 'tp'), may hold values from -0.125 to 0.125
- dense_down: bfloat16 [1024, 2048], P('tp'), may hold values from -0.1875 to 0.1875
Outputs:
- mixed: bfloat16 [128, 2048], P('ep', 'tp')
The draws below stay inside these ranges and needn't reach their ends.
Inputs may be any that keep to these rules, and one draw needn't show every extreme that they name: `cum_gate`: along positions each row never rises: entry p is the sum of the log forget gates of positions 0 to p of that sequence and head. `chosen`: each row names two different experts of one group of 8 consecutive expert numbers. The rows of one device name any one expert at most 8 times, and some expert exactly 8 times.
All inputs are finite; a program needn't handle non-finite values.
Results may differ from the reference program's by a relative error of at most 0.014.
Values may be sent and summed in bfloat16 or wider, within the bound.
A program may use at most 64 MiB of HBM per device.

```python
import jax
import jax.numpy as jnp
from jax import lax

D = 2048
QUERY_HEADS = 16
KVH = 4
HD = 64
DE = 1024
DF = 1024
EPG = 8
TOP = 2
CACHED_POSITIONS = 1024
SEQ_DEV = 16
SEQUENCE_TOTAL = 128
EXPERTS = 8
CAP = 8
N_EP = 8
N_TP = 4


def draw_tokens(key, part):
    first, second, third = jax.random.split(key, 3)
    column_pos = jnp.arange(D, dtype=jnp.float32) / D
    entries = jax.random.normal(first, (SEQUENCE_TOTAL, D), jnp.float32)
    column_scale = 3.0 ** column_pos
    row_scale = jnp.exp(jax.random.uniform(second, (SEQUENCE_TOTAL, 1), jnp.float32, jnp.log(0.5), jnp.log(2.0)))
    roughness = jnp.exp(jax.random.uniform(third, (1, D), jnp.float32, jnp.log(0.5), jnp.log(2.0)))
    return (entries * 0.6 * column_scale[None, :] * roughness * row_scale).astype(jnp.bfloat16)


def draw_kv_cache(key, part):
    first = jax.random.fold_in(key, 0)
    total_width = 2 * KVH * HD
    entries = jax.random.normal(first, (SEQUENCE_TOTAL, CACHED_POSITIONS, total_width), jnp.float32)
    return entries.astype(jnp.bfloat16)


def draw_cum_gate(key, part):
    key_rows = jax.random.split(key, 7)
    scores_int = jax.random.randint(key_rows[0], (SEQUENCE_TOTAL, QUERY_HEADS), 0, 2 ** 20) * QUERY_HEADS + jnp.arange(QUERY_HEADS, dtype=jnp.int32)[None, :]
    ranking = jnp.argsort(jnp.argsort(scores_int, axis=1), axis=1)
    slow_count = QUERY_HEADS // 2
    slow = (ranking < slow_count)[:, :, None]
    slow_rate = jnp.exp(jax.random.uniform(key_rows[1], (SEQUENCE_TOTAL, QUERY_HEADS, 1), jnp.float32, jnp.log(0.2), jnp.log(0.8))) / CACHED_POSITIONS
    fast_rate = jnp.exp(jax.random.uniform(key_rows[2], (SEQUENCE_TOTAL, QUERY_HEADS, 1), jnp.float32, jnp.log(0.01), jnp.log(1.0 / 30.0)))
    rate_all = jnp.where(slow, slow_rate, fast_rate)
    block_factor = jnp.exp(jax.random.uniform(key_rows[3], (SEQUENCE_TOTAL, 1, CACHED_POSITIONS // 128), jnp.float32, jnp.log(0.5), jnp.log(2.0)))
    block_factor = jnp.repeat(block_factor, 128, axis=2)
    roughness = jnp.exp(jax.random.uniform(key_rows[4], (SEQUENCE_TOTAL, QUERY_HEADS, CACHED_POSITIONS), jnp.float32, jnp.log(0.5), jnp.log(2.0)))
    stepping_through = -rate_all * block_factor * roughness
    group_position = jax.random.randint(key_rows[5], (SEQUENCE_TOTAL, QUERY_HEADS, 2), 0, CACHED_POSITIONS)
    group_length = jnp.log(jax.random.uniform(key_rows[6], (SEQUENCE_TOTAL, QUERY_HEADS, 2), jnp.float32, 0.5, 0.8))
    position_rows = jnp.arange(CACHED_POSITIONS, dtype=jnp.int32)
    position_groups = jnp.sum(jnp.where(position_rows[None, None, None, :] == group_position[:, :, :, None], group_length[:, :, :, None], 0.0), axis=2)
    return jnp.cumsum(stepping_through + position_groups, axis=-1).astype(jnp.float32)


def draw_chosen(key, part):
    pair_count = EXPERTS // 2

    def one_block(block_key):
        key_perm, key_first, key_rest, key_order = jax.random.split(block_key, 4)
        group_keys = jax.random.split(key_perm, EXPERTS // EPG)

        def shuffle_group(group_key):
            return jax.random.permutation(group_key, EPG).astype(jnp.int32)
        shuffled = jax.vmap(shuffle_group)(group_keys)
        offsets = (jnp.arange(EXPERTS // EPG, dtype=jnp.int32) * EPG)[:, None]
        members = (shuffled + offsets).reshape(pair_count, 2).astype(jnp.int32)
        first_pair = jax.random.randint(key_first, (), 0, pair_count).astype(jnp.int32)
        others = (jax.random.permutation(key_rest, (pair_count - 1) * CAP)[:SEQ_DEV - CAP] // CAP).astype(jnp.int32)
        others = others + (others >= first_pair).astype(jnp.int32)
        pairs = jnp.concatenate([jnp.full((CAP,), first_pair, jnp.int32), others])
        pairs = pairs[jax.random.permutation(key_order, SEQ_DEV)]
        return members[pairs]
    block_keys = jax.random.split(key, N_EP)
    return jax.vmap(one_block)(block_keys).reshape(SEQ_DEV * N_EP, TOP).astype(jnp.int32)


def with_ends(result, rng, smallest, high):
    longest = result.shape.index(max(result.shape))
    spots = []
    for shift in (0, 1):
        where = [jax.random.randint(jax.random.fold_in(rng, axis), (), 0, length) for axis, length in enumerate(result.shape)]
        where[longest] = (where[longest] + shift) % result.shape[longest]
        spots.append(tuple(where))
    return result.at[spots[0]].set(smallest).at[spots[1]].set(high)


def level_of(own_key, extent, pieces, smallest, high):
    level, own = 1.0, jax.random.fold_in(own_key, 6)
    for axis_at, shards_of in pieces:
        draws = jnp.exp(jax.random.uniform(jax.random.fold_in(own, axis_at), (shards_of,), jnp.float32, smallest / len(pieces), high / len(pieces)))
        level = level * jnp.repeat(draws, extent[axis_at] // shards_of).reshape([-1 if axis == axis_at else 1 for axis in range(len(extent))])
    return level


def normal_values(own_key, extent, width, reach, cuts=(), kind=jnp.bfloat16):
    array = jax.random.normal(own_key, extent, jnp.float32) * width
    if len(cuts) > 0:
        array = level_of(own_key, extent, cuts, -0.22, 0.18) * array
    return jnp.clip(array, min=-reach, max=reach).astype(kind)


def setup_inputs(seed: int = 0) -> dict:
    key_of = jax.random.split(jax.random.key(seed), 22)
    tokens = draw_tokens(jax.random.fold_in(key_of[21], 71), 0)
    kv_cache = draw_kv_cache(jax.random.fold_in(key_of[21], 71), 0)
    cum_gate = draw_cum_gate(jax.random.fold_in(key_of[21], 71), 0)
    lengths = with_ends(jax.random.randint(key_of[3], (SEQUENCE_TOTAL,), CACHED_POSITIONS // 4, CACHED_POSITIONS + 1), jax.random.fold_in(key_of[3], 1), CACHED_POSITIONS // 4, CACHED_POSITIONS).astype(jnp.int32)
    w_query = normal_values(key_of[4], (D, QUERY_HEADS * HD), D ** -0.5, 0.125, ((1, 4),))
    w_key = normal_values(key_of[5], (D, KVH * HD), D ** -0.5, 0.125, ((1, 4),))
    w_value = normal_values(key_of[6], (D, KVH * HD), D ** -0.5, 0.125, ((1, 4),))
    w_forget = normal_values(key_of[7], (D, QUERY_HEADS), (D // 16) ** -0.5, 0.5, ((1, 4),))
    forget_bias = jnp.clip(-2.5 + 4.0 * jax.random.uniform(key_of[8], (QUERY_HEADS,), jnp.float32) ** level_of(key_of[8], (QUERY_HEADS,), ((0, 4),), -0.2, 0.2), -2.5, 1.5)
    w_out = normal_values(key_of[9], (QUERY_HEADS * HD, D), (QUERY_HEADS * HD) ** -0.5, 0.1875, ((0, 4),))
    attn_gain = jnp.clip(1.0 + 0.18 * jax.random.normal(key_of[10], (D,), jnp.float32), 0.099609375, 1.8984375).astype(jnp.bfloat16)
    ffn_gain = jnp.clip(1.0 + 0.18 * jax.random.normal(key_of[11], (D,), jnp.float32), 0.099609375, 1.8984375).astype(jnp.bfloat16)
    mix_gate = normal_values(key_of[12], (D,), D ** -0.5, 0.125)
    expert_gate = normal_values(key_of[13], (EXPERTS, D, DE), D ** -0.5, 0.125, ((0, 8), (2, 4)))
    expert_up = normal_values(key_of[14], (EXPERTS, D, DE), D ** -0.5, 0.125, ((0, 8), (2, 4)))
    expert_down = normal_values(key_of[15], (EXPERTS, DE, D), DE ** -0.5, 0.1875, ((0, 8), (1, 4)))
    chosen = draw_chosen(jax.random.fold_in(key_of[21], 71), 0)
    route_weight = jnp.clip(0.5 + 1.0 * jax.random.uniform(key_of[17], (SEQUENCE_TOTAL, TOP), jnp.float32) ** level_of(key_of[17], (SEQUENCE_TOTAL, TOP), ((0, 8),), -0.2, 0.2), 0.5, 1.5)
    dense_gate = normal_values(key_of[18], (D, DF), D ** -0.5, 0.125, ((1, 4),))
    dense_up = normal_values(key_of[19], (D, DF), D ** -0.5, 0.125, ((1, 4),))
    dense_down = normal_values(key_of[20], (DF, D), DF ** -0.5, 0.1875, ((0, 4),))
    return {"tokens": tokens, "kv_cache": kv_cache, "cum_gate": cum_gate, "lengths": lengths, "w_query": w_query, "w_key": w_key, "w_value": w_value, "w_forget": w_forget, "forget_bias": forget_bias, "w_out": w_out, "attn_gain": attn_gain, "ffn_gain": ffn_gain, "mix_gate": mix_gate, "expert_gate": expert_gate, "expert_up": expert_up, "expert_down": expert_down, "chosen": chosen, "route_weight": route_weight, "dense_gate": dense_gate, "dense_up": dense_up, "dense_down": dense_down}


epsilon = 1e-06

def norm_rows(values, scales):
    widened = values.astype(jnp.float32)
    square = lax.optimization_barrier(jnp.mean(widened * widened, axis=-1, keepdims=True))
    return (widened * lax.rsqrt(square + epsilon) * scales.astype(jnp.float32)).astype(jnp.bfloat16)

def split_sum(left, right):
    piece_width = left.shape[1] // N_TP
    running = jnp.zeros((left.shape[0], right.shape[1]), jnp.float32)
    for member in range(N_TP):
        lower = member * piece_width
        partial_value = jnp.dot(left[:, lower:lower + piece_width], right[lower:lower + piece_width], preferred_element_type=jnp.float32).astype(jnp.bfloat16)
        partial_value = lax.optimization_barrier(partial_value)
        running = running + partial_value.astype(jnp.float32)
    return running

def reference(tokens, kv_cache, cum_gate, lengths, w_query, w_key, w_value, w_forget, forget_bias, w_out, attn_gain, ffn_gain, mix_gate, expert_gate, expert_up, expert_down, chosen, route_weight, dense_gate, dense_up, dense_down):
    group_size = QUERY_HEADS // KVH
    score_scale = HD ** (-0.5)
    h_one = norm_rows(tokens, attn_gain)
    queries = jnp.dot(h_one, w_query, preferred_element_type=jnp.float32).astype(jnp.bfloat16)
    key_new = jnp.dot(h_one, w_key, preferred_element_type=jnp.float32).astype(jnp.bfloat16)
    value_new = jnp.dot(h_one, w_value, preferred_element_type=jnp.float32).astype(jnp.bfloat16)
    log_forget = jax.nn.log_sigmoid(jnp.dot(h_one, w_forget, preferred_element_type=jnp.float32) + forget_bias)

    def one_sequence(packed):
        query_row, key_row, value_row, forget_row, cache_row, gate_row, length_one = packed
        query_heads = query_row.astype(jnp.float32).reshape(KVH, group_size, HD)
        stacked = cache_row.astype(jnp.float32).reshape(CACHED_POSITIONS, KVH, 2, HD)
        scores = jnp.einsum('jgd,cjd->jgc', query_heads, stacked[:, :, 0, :]) * score_scale
        gate_rows = gate_row.reshape(KVH, group_size, CACHED_POSITIONS)
        latest = lax.dynamic_index_in_dim(gate_rows, (length_one - 1).astype(jnp.int32), axis=2, keepdims=True)
        scores = scores + latest - gate_rows + forget_row.reshape(KVH, group_size)[:, :, None]
        position_rows = jnp.arange(CACHED_POSITIONS, dtype=jnp.int32)
        scores = jnp.where(position_rows[None, None, :] < length_one, scores, -jnp.inf)
        own_score = jnp.einsum('jgd,jd->jg', query_heads, key_row.astype(jnp.float32).reshape(KVH, HD)) * score_scale
        highest = jnp.maximum(lax.optimization_barrier(jnp.max(scores, axis=-1)), own_score)
        weights = jnp.exp(scores - highest[:, :, None])
        own_weight = jnp.exp(own_score - highest)
        denominator = lax.optimization_barrier(jnp.sum(weights, axis=-1)) + own_weight
        weights = (weights / denominator[:, :, None]).astype(jnp.bfloat16)
        own_weight = (own_weight / denominator).astype(jnp.bfloat16)
        blended = jnp.einsum('jgc,cjd->jgd', weights.astype(jnp.float32), stacked[:, :, 1, :])
        blended = blended + own_weight.astype(jnp.float32)[:, :, None] * value_row.astype(jnp.float32).reshape(KVH, 1, HD)
        return blended.astype(jnp.bfloat16).reshape(QUERY_HEADS * HD)
    head_out = lax.map(one_sequence, (queries, key_new, value_new, log_forget, kv_cache, cum_gate, lengths))
    attention = split_sum(head_out, w_out)
    residual = (tokens.astype(jnp.float32) + attention).astype(jnp.bfloat16)
    h_two = norm_rows(residual, ffn_gain)
    flat_routes = chosen.reshape(N_EP, SEQ_DEV * TOP)
    one_hot = (flat_routes[:, :, None] == jnp.arange(EXPERTS, dtype=jnp.int32)[None, None, :]).astype(jnp.int32)
    earlier = (jnp.cumsum(one_hot, axis=1) - one_hot).astype(jnp.int32)
    rank_of = lax.optimization_barrier(jnp.sum(earlier * one_hot, axis=-1)).astype(jnp.int32)
    slot_of = (jnp.arange(N_EP, dtype=jnp.int32)[:, None] * CAP + rank_of).reshape(-1).astype(jnp.int32)
    expert_of = flat_routes.reshape(-1).astype(jnp.int32)
    source_rows = (jnp.arange(SEQUENCE_TOTAL * TOP, dtype=jnp.int32) // TOP).astype(jnp.int32)
    buffer = jnp.zeros((EXPERTS, N_EP * CAP, D), jnp.bfloat16).at[expert_of, slot_of].set(h_two[source_rows])

    def run_expert(packed):
        inputs_here, gate_here, up_here, down_here = packed
        gate_pre = jnp.dot(inputs_here, gate_here, preferred_element_type=jnp.float32)
        up_pre = jnp.dot(inputs_here, up_here, preferred_element_type=jnp.float32)
        hidden = (jax.nn.silu(gate_pre) * up_pre).astype(jnp.bfloat16)
        return split_sum(hidden, down_here).astype(jnp.bfloat16)
    expert_rows = lax.map(run_expert, (buffer, expert_gate, expert_up, expert_down))
    picked = expert_rows[expert_of, slot_of].astype(jnp.float32).reshape(SEQUENCE_TOTAL, TOP, D)
    routed_sum = lax.optimization_barrier(jnp.sum(picked * route_weight[:, :, None], axis=1))
    dense_pre = jnp.dot(h_two, dense_gate, preferred_element_type=jnp.float32)
    dense_lift = jnp.dot(h_two, dense_up, preferred_element_type=jnp.float32)
    dense_act = (jax.nn.silu(dense_pre) * dense_lift).astype(jnp.bfloat16)
    dense_out = split_sum(dense_act, dense_down)
    blend_gate = jax.nn.sigmoid(jnp.dot(h_two, mix_gate, preferred_element_type=jnp.float32))
    return (residual.astype(jnp.float32) + routed_sum + blend_gate[:, None] * dense_out).astype(jnp.bfloat16)
```

```python
import functools

import jax
import jax.numpy as jnp
from jax import lax
from jax.experimental import pallas as pl
from jax.experimental.pallas import tpu as pltpu
from jax.sharding import PartitionSpec as P

HD = 64
TOP = 2
MESH = pl.DeviceIdType.MESH
F32 = jnp.float32
BF16 = jnp.bfloat16
epsilon = 1e-06


def dot(a, b):
    return jnp.dot(a, b, preferred_element_type=F32)


def norm_rows(widened, scales):
    square = jnp.mean(widened * widened, axis=-1, keepdims=True)
    return (widened * lax.rsqrt(square + epsilon) * scales.astype(F32)).astype(BF16)


def kernel(
    n_ep,
    n_tp,
    cap,
    tokens,
    lengths,
    forget_bias,
    attn_gain,
    ffn_gain,
    mix_gate,
    chosen,
    route_weight,
    kv_hbm,
    cum_hbm,
    wq_hbm,
    wk_hbm,
    wv_hbm,
    wf_hbm,
    wo_hbm,
    eg_hbm,
    eu_hbm,
    ed_hbm,
    dg_hbm,
    du_hbm,
    dd_hbm,
    out,
    kv,
    cum,
    wq,
    wk,
    wv,
    wf,
    wo,
    eg,
    eu,
    ed,
    dg,
    du,
    dd,
    load_sem,
    kv_sem,
    gathered,
    q3,
    f3,
    kvn,
    o3,
    att_out,
    att_in,
    disp_out,
    disp_in,
    dense_send,
    dense_recv,
    exp_send,
    exp_recv,
    ret_out,
    ret_in,
    tp_send,
    tp_recv,
    ep_send,
    ep_recv,
):
    me_tp = lax.axis_index("tp")
    me_ep = lax.axis_index("ep")
    seqs, width = tokens.shape
    heads = cum.shape[1]
    cache_len = kv.shape[1]
    rows = n_ep * cap

    loads = {}
    for spot, (name, src, dst) in enumerate(
        (
            ("wq", wq_hbm, wq),
            ("wk", wk_hbm, wk),
            ("wv", wv_hbm, wv),
            ("wf", wf_hbm, wf),
            ("cum", cum_hbm, cum),
        )
    ):
        loads[name] = pltpu.make_async_copy(src, dst, load_sem.at[spot])
        loads[name].start()
    kv_parts = kv_sem.shape[0]
    part = seqs // kv_parts
    kv_loads = []
    for piece in range(kv_parts):
        span = pl.ds(piece * part, part)
        kv_loads.append(
            pltpu.make_async_copy(kv_hbm.at[span], kv.at[span], kv_sem.at[piece])
        )
        kv_loads[-1].start()
    for spot, (name, src, dst) in enumerate(
        (
            ("wo", wo_hbm, wo),
            ("dg", dg_hbm, dg),
            ("du", du_hbm, du),
            ("dd", dd_hbm, dd),
            ("eg", eg_hbm.at[0], eg),
            ("eu", eu_hbm.at[0], eu),
            ("ed", ed_hbm.at[0], ed),
        )
    ):
        loads[name] = pltpu.make_async_copy(src, dst, load_sem.at[5 + spot])
        loads[name].start()

    barrier = pltpu.get_barrier_semaphore()
    for step in range(1, n_tp):
        pl.semaphore_signal(
            barrier,
            inc=1,
            device_id={"tp": lax.rem(me_tp + step, n_tp)},
            device_id_type=MESH,
        )

    def greet(step, carry):
        pl.semaphore_signal(
            barrier,
            inc=1,
            device_id={"ep": lax.rem(me_ep + step, n_ep)},
            device_id_type=MESH,
        )
        return carry

    lax.fori_loop(1, n_ep, greet, 0)
    pl.semaphore_wait(barrier, n_tp - 1 + n_ep - 1)

    def tp_copy(phase, step, src, dst):
        return pltpu.make_async_remote_copy(
            src_ref=src,
            dst_ref=dst,
            send_sem=tp_send.at[phase, step],
            recv_sem=tp_recv.at[phase, step],
            device_id={"tp": lax.rem(me_tp + step, n_tp)},
            device_id_type=MESH,
        )

    def ep_copy(phase, step, src, dst):
        return pltpu.make_async_remote_copy(
            src_ref=src,
            dst_ref=dst,
            send_sem=ep_send.at[phase, step],
            recv_sem=ep_recv.at[phase, step],
            device_id={"ep": lax.rem(me_ep + step, n_ep)},
            device_id_type=MESH,
        )

    token_copies = [
        tp_copy(0, step, tokens, gathered.at[me_tp]) for step in range(1, n_tp)
    ]
    for copy in token_copies:
        copy.start()
    gathered[me_tp] = tokens[...]

    slot = lax.broadcasted_iota(jnp.int32, (seqs, rows), 1)
    slot_expert = slot // cap
    slot_place = (slot % cap).astype(F32)
    first = (chosen[:, 0:1] == slot_expert).astype(F32)
    second = (chosen[:, 1:2] == slot_expert).astype(F32)
    either = first + second
    earlier = (
        lax.broadcasted_iota(jnp.int32, (seqs, seqs), 1)
        < lax.broadcasted_iota(jnp.int32, (seqs, seqs), 0)
    ).astype(F32)
    rank = dot(earlier.astype(BF16), either.astype(BF16))
    in_place = (rank == slot_place).astype(F32)
    first = (first * in_place).astype(BF16)
    second = (second * in_place).astype(BF16)
    either = either * in_place

    for copy in token_copies:
        copy.wait()
    tokens_full = jnp.concatenate(
        [gathered[member].astype(F32) for member in range(n_tp)], axis=1
    )
    h_one = norm_rows(tokens_full, attn_gain[...])

    for name in ("wq", "wk", "wv", "wf"):
        loads[name].wait()
    queries = dot(h_one, wq[...]).astype(BF16).astype(F32)
    key_new = dot(h_one, wk[...]).astype(BF16).astype(F32)
    value_new = dot(h_one, wv[...]).astype(BF16).astype(F32)
    forget_pre = dot(h_one, wf[...]) + forget_bias[...]
    forget_now = jnp.minimum(forget_pre, 0.0) - jnp.log1p(
        jnp.exp(-jnp.abs(forget_pre))
    )
    blank = jnp.zeros((seqs, HD), F32)
    for head in range(heads):
        q3[:, head, :] = jnp.concatenate(
            [queries[:, head * HD : (head + 1) * HD], blank], axis=1
        )
        f3[:, head, :] = jnp.broadcast_to(forget_now[:, head : head + 1], (seqs, 2 * HD))
    kvn[...] = jnp.concatenate([key_new, value_new], axis=1)

    score_scale = HD ** (-0.5)
    position = lax.broadcasted_iota(jnp.int32, (heads, cache_len), 1)
    loads["cum"].wait()

    def attend(seq):
        length = lengths[seq]
        query = q3[seq]
        entries = kv[seq]
        scores = (
            lax.dot_general(
                query.astype(BF16),
                entries,
                (((1,), (1,)), ((), ())),
                preferred_element_type=F32,
            )
            * score_scale
        )
        gates = cum[seq]
        latest = jnp.sum(
            jnp.where(position == length - 1, gates, 0.0), axis=1, keepdims=True
        )
        scores = scores - gates + (latest + f3[seq][:, 0:1])
        scores = jnp.where(position < length, scores, -jnp.inf)
        new_row = kvn[pl.ds(seq, 1), :]
        own_score = jnp.sum(query * new_row, axis=1, keepdims=True) * score_scale
        highest = jnp.maximum(jnp.max(scores, axis=1, keepdims=True), own_score)
        weights = jnp.exp(scores - highest)
        own_weight = jnp.exp(own_score - highest)
        inverse = 1.0 / (jnp.sum(weights, axis=1, keepdims=True) + own_weight)
        blended = dot((weights * inverse).astype(BF16), entries)
        own_weight = (own_weight * inverse).astype(BF16).astype(F32)
        o3[seq] = blended + own_weight * new_row

    for piece in range(kv_parts):
        kv_loads[piece].wait()
        for seq in range(piece * part, (piece + 1) * part):
            attend(seq)
    head_out = jnp.concatenate(
        [o3[:, head, :][:, HD:] for head in range(heads)], axis=1
    ).astype(BF16)

    loads["wo"].wait()
    att_out[...] = dot(head_out, wo[...]).astype(BF16)
    att_copies = [tp_copy(1, step, att_out, att_in.at[step]) for step in range(1, n_tp)]
    for copy in att_copies:
        copy.start()
    attention = att_out[...].astype(F32)
    for step in range(1, n_tp):
        att_copies[step - 1].wait()
        attention = attention + att_in[step].astype(F32)
    residual_full = (tokens_full + attention).astype(BF16)
    h_two = norm_rows(residual_full.astype(F32), ffn_gain[...])
    for member in range(n_tp):
        gathered[member] = residual_full[:, member * width : (member + 1) * width]

    outgoing = dot(jnp.transpose(either).astype(BF16), h_two)
    disp_out[...] = outgoing.reshape(n_ep, cap, n_tp * width).astype(BF16)

    def dispatch(step, carry):
        ep_copy(
            0, step, disp_out.at[lax.rem(me_ep + step, n_ep)], disp_in.at[me_ep]
        ).start()
        return carry

    lax.fori_loop(1, n_ep, dispatch, 0)
    disp_in[me_ep] = disp_out[me_ep]

    for name in ("dg", "du", "dd"):
        loads[name].wait()
    dense_pre = dot(h_two, dg[...])
    dense_act = (dense_pre * jax.nn.sigmoid(dense_pre) * dot(h_two, du[...])).astype(BF16)
    dense_part = dot(dense_act, dd[...]).astype(BF16)
    for member in range(n_tp):
        dense_send[member] = dense_part[:, member * width : (member + 1) * width]
    dense_copies = [
        tp_copy(
            2, step, dense_send.at[lax.rem(me_tp + step, n_tp)], dense_recv.at[step]
        )
        for step in range(1, n_tp)
    ]
    for copy in dense_copies:
        copy.start()
    blend_gate = jax.nn.sigmoid(
        jnp.sum(h_two.astype(F32) * mix_gate[...].astype(F32), axis=1, keepdims=True)
    )

    def dispatched(step, carry):
        ep_copy(
            0, step, disp_out.at[lax.rem(me_ep + step, n_ep)], disp_in.at[me_ep]
        ).wait()
        return carry

    for name in ("eg", "eu", "ed"):
        loads[name].wait()
    lax.fori_loop(1, n_ep, dispatched, 0)

    flat_rows = disp_in[...].astype(F32).reshape(rows, n_tp * width).astype(BF16)
    gate_pre = dot(flat_rows, eg[...])
    hidden = (gate_pre * jax.nn.sigmoid(gate_pre) * dot(flat_rows, eu[...])).astype(BF16)
    exp_copies = []
    for step in list(range(1, n_tp)) + [0]:
        target = lax.rem(me_tp + step, n_tp)
        columns = pl.ds(pl.multiple_of(target * width, width), width)
        exp_send[step] = dot(hidden, ed[:, columns]).astype(BF16)
        if step > 0:
            exp_copies.append(tp_copy(3, step, exp_send.at[step], exp_recv.at[step]))
            exp_copies[-1].start()
    dense_out = dense_send[me_tp].astype(F32)
    for step in range(1, n_tp):
        dense_copies[step - 1].wait()
        dense_out = dense_out + dense_recv[step].astype(F32)
    base = gathered[me_tp].astype(F32) + blend_gate * dense_out
    shares = exp_send[0].astype(F32)
    for step in range(1, n_tp):
        exp_copies[step - 1].wait()
        shares = shares + exp_recv[step].astype(F32)

    ret_out[...] = shares.reshape(n_ep, cap, width).astype(BF16)

    def give_back(step, carry):
        ep_copy(
            1, step, ret_out.at[lax.rem(me_ep + step, n_ep)], ret_in.at[me_ep]
        ).start()
        return carry

    lax.fori_loop(1, n_ep, give_back, 0)
    ret_in[me_ep] = ret_out[me_ep]

    def given_back(step, carry):
        ep_copy(
            1, step, ret_out.at[lax.rem(me_ep + step, n_ep)], ret_in.at[me_ep]
        ).wait()
        return carry

    lax.fori_loop(1, n_ep, given_back, 0)
    returned = ret_in[...].astype(F32).reshape(rows, width).astype(BF16)
    routed = dot(first, returned) * route_weight[:, 0:1]
    routed = routed + dot(second, returned) * route_weight[:, 1:2]
    out[...] = (base + routed).astype(BF16)


def local(
    n_ep,
    n_tp,
    tokens,
    kv_cache,
    cum_gate,
    lengths,
    w_query,
    w_key,
    w_value,
    w_forget,
    forget_bias,
    w_out,
    attn_gain,
    ffn_gain,
    mix_gate,
    expert_gate,
    expert_up,
    expert_down,
    chosen,
    route_weight,
    dense_gate,
    dense_up,
    dense_down,
):
    seqs, width = tokens.shape
    model = n_tp * width
    heads = w_query.shape[1] // HD
    assert w_key.shape[1] == HD
    cap = max(2, (4 * seqs + n_ep - 1) // n_ep)
    cap = (cap + 7) // 8 * 8
    rows = n_ep * cap
    vmem = pl.BlockSpec(memory_space=pltpu.VMEM)
    smem = pl.BlockSpec(memory_space=pltpu.SMEM)
    hbm = pl.BlockSpec(memory_space=pl.ANY)
    like = lambda a: pltpu.VMEM(a.shape, a.dtype)
    return pl.pallas_call(
        functools.partial(kernel, n_ep, n_tp, cap),
        out_shape=jax.ShapeDtypeStruct((seqs, width), BF16),
        in_specs=[vmem, smem] + [vmem] * 6 + [hbm] * 13,
        out_specs=vmem,
        scratch_shapes=[
            like(kv_cache),
            like(cum_gate),
            like(w_query),
            like(w_key),
            like(w_value),
            like(w_forget),
            like(w_out),
            like(expert_gate[0]),
            like(expert_up[0]),
            like(expert_down[0]),
            like(dense_gate),
            like(dense_up),
            like(dense_down),
            pltpu.SemaphoreType.DMA((12,)),
            pltpu.SemaphoreType.DMA((4,)),
            pltpu.VMEM((n_tp, seqs, width), BF16),
            pltpu.VMEM((seqs, heads, 2 * HD), F32),
            pltpu.VMEM((seqs, heads, 2 * HD), F32),
            pltpu.VMEM((seqs, 2 * HD), F32),
            pltpu.VMEM((seqs, heads, 2 * HD), F32),
            pltpu.VMEM((seqs, model), BF16),
            pltpu.VMEM((n_tp, seqs, model), BF16),
            pltpu.VMEM((n_ep, cap, model), BF16),
            pltpu.VMEM((n_ep, cap, model), BF16),
            pltpu.VMEM((n_tp, seqs, width), BF16),
            pltpu.VMEM((n_tp, seqs, width), BF16),
            pltpu.VMEM((n_tp, rows, width), BF16),
            pltpu.VMEM((n_tp, rows, width), BF16),
            pltpu.VMEM((n_ep, cap, width), BF16),
            pltpu.VMEM((n_ep, cap, width), BF16),
            pltpu.SemaphoreType.DMA((4, n_tp)),
            pltpu.SemaphoreType.DMA((4, n_tp)),
            pltpu.SemaphoreType.DMA((2, n_ep)),
            pltpu.SemaphoreType.DMA((2, n_ep)),
        ],
        compiler_params=pltpu.CompilerParams(
            collective_id=0,
            has_side_effects=True,
            vmem_limit_bytes=60 * 1024 * 1024,
        ),
    )(
        tokens,
        lengths,
        forget_bias.reshape(1, -1),
        attn_gain.reshape(1, -1),
        ffn_gain.reshape(1, -1),
        mix_gate.reshape(1, -1),
        chosen,
        route_weight,
        kv_cache,
        cum_gate,
        w_query,
        w_key,
        w_value,
        w_forget,
        w_out,
        expert_gate,
        expert_up,
        expert_down,
        dense_gate,
        dense_up,
        dense_down,
    )


def solution(mesh):
    in_specs = (
        P("ep", "tp"),
        P("ep", None, "tp"),
        P("ep", "tp", None),
        P("ep"),
        P(None, "tp"),
        P(None, "tp"),
        P(None, "tp"),
        P(None, "tp"),
        P("tp"),
        P("tp", None),
        P(),
        P(),
        P(),
        P("ep", None, "tp"),
        P("ep", None, "tp"),
        P("ep", "tp", None),
        P("ep", None),
        P("ep", None),
        P(None, "tp"),
        P(None, "tp"),
        P("tp", None),
    )
    out_specs = P("ep", "tp")
    return jax.shard_map(
        functools.partial(local, mesh.shape["ep"], mesh.shape["tp"]),
        mesh=mesh,
        in_specs=in_specs,
        out_specs=out_specs,
        check_vma=False,
    )
```

```python
import functools

import jax
import jax.numpy as jnp
from jax import lax
from jax.experimental import pallas as pl
from jax.experimental.pallas import tpu as pltpu
from jax.sharding import PartitionSpec as P

HD = 64
TOP = 2
MESH = pl.DeviceIdType.MESH
F32 = jnp.float32
BF16 = jnp.bfloat16
epsilon = 1e-06


def dot(a, b):
    return jnp.dot(a, b, preferred_element_type=F32)


def dot_t(a, b):
    return lax.dot_general(a, b, (((1,), (1,)), ((), ())), preferred_element_type=F32)


def norm_rows(widened, scales):
    square = jnp.mean(widened * widened, axis=-1, keepdims=True)
    return (widened * lax.rsqrt(square + epsilon) * scales.astype(F32)).astype(BF16)


def kernel(
    n_ep,
    n_tp,
    cap,
    tokens,
    lengths,
    forget_bias,
    attn_gain,
    ffn_gain,
    mix_gate,
    chosen,
    route_weight,
    kv_hbm,
    cum_hbm,
    wq_hbm,
    wk_hbm,
    wv_hbm,
    wf_hbm,
    wo_hbm,
    eg_hbm,
    eu_hbm,
    ed_hbm,
    dg_hbm,
    du_hbm,
    dd_hbm,
    out,
    kv,
    cum,
    wq,
    wk,
    wv,
    wf,
    wo,
    eg,
    eu,
    ed,
    dg,
    du,
    dd,
    load_sem,
    kv_sem,
    gathered,
    q3,
    f3,
    kvn,
    o3,
    att_out,
    att_in,
    disp_out,
    disp_in,
    dense_send,
    dense_recv,
    exp_send,
    exp_recv,
    ret_out,
    ret_in,
    tp_send,
    tp_recv,
    ep_send,
    ep_recv,
):
    me_tp = lax.axis_index("tp")
    me_ep = lax.axis_index("ep")
    seqs, width = tokens.shape
    heads = cum.shape[1]
    cache_len = kv.shape[1]
    rows = n_ep * cap

    loads = {}
    for spot, (name, src, dst) in enumerate(
        (
            ("wq", wq_hbm, wq),
            ("wk", wk_hbm, wk),
            ("wv", wv_hbm, wv),
            ("wf", wf_hbm, wf),
            ("cum", cum_hbm, cum),
        )
    ):
        loads[name] = pltpu.make_async_copy(src, dst, load_sem.at[spot])
        loads[name].start()
    kv_parts = kv_sem.shape[0]
    part = seqs // kv_parts
    kv_loads = []
    for piece in range(kv_parts):
        span = pl.ds(piece * part, part)
        kv_loads.append(
            pltpu.make_async_copy(kv_hbm.at[span], kv.at[span], kv_sem.at[piece])
        )
        kv_loads[-1].start()
    for spot, (name, src, dst) in enumerate(
        (
            ("wo", wo_hbm, wo),
            ("dg", dg_hbm, dg),
            ("du", du_hbm, du),
            ("dd", dd_hbm, dd),
            ("eg", eg_hbm.at[0], eg),
            ("eu", eu_hbm.at[0], eu),
            ("ed", ed_hbm.at[0], ed),
        )
    ):
        loads[name] = pltpu.make_async_copy(src, dst, load_sem.at[5 + spot])
        loads[name].start()

    barrier = pltpu.get_barrier_semaphore()
    for step in range(1, n_tp):
        pl.semaphore_signal(
            barrier,
            inc=1,
            device_id={"tp": lax.rem(me_tp + step, n_tp)},
            device_id_type=MESH,
        )

    def greet(step, carry):
        pl.semaphore_signal(
            barrier,
            inc=1,
            device_id={"ep": lax.rem(me_ep + step, n_ep)},
            device_id_type=MESH,
        )
        return carry

    lax.fori_loop(1, n_ep, greet, 0)
    pl.semaphore_wait(barrier, n_tp - 1 + n_ep - 1)

    def tp_copy(phase, step, src, dst):
        return pltpu.make_async_remote_copy(
            src_ref=src,
            dst_ref=dst,
            send_sem=tp_send.at[phase, step],
            recv_sem=tp_recv.at[phase, step],
            device_id={"tp": lax.rem(me_tp + step, n_tp)},
            device_id_type=MESH,
        )

    def ep_copy(phase, step, src, dst):
        return pltpu.make_async_remote_copy(
            src_ref=src,
            dst_ref=dst,
            send_sem=ep_send.at[phase, step],
            recv_sem=ep_recv.at[phase, step],
            device_id={"ep": lax.rem(me_ep + step, n_ep)},
            device_id_type=MESH,
        )

    token_copies = [
        tp_copy(0, step, tokens, gathered.at[me_tp]) for step in range(1, n_tp)
    ]
    for copy in token_copies:
        copy.start()
    gathered[me_tp] = tokens[...]

    slot = lax.broadcasted_iota(jnp.int32, (rows, seqs), 0)
    slot_expert = slot // cap
    slot_place = (slot % cap).astype(F32)
    first = (chosen[0:1, :] == slot_expert).astype(F32)
    second = (chosen[1:2, :] == slot_expert).astype(F32)
    either = first + second
    earlier = (
        lax.broadcasted_iota(jnp.int32, (seqs, seqs), 0)
        < lax.broadcasted_iota(jnp.int32, (seqs, seqs), 1)
    ).astype(F32)
    rank = dot(either.astype(BF16), earlier.astype(BF16))
    in_place = (rank == slot_place).astype(F32)
    either = (either * in_place).astype(BF16)
    weighted = first * route_weight[0:1, :] + second * route_weight[1:2, :]
    weighted = jnp.transpose(weighted * in_place)
    high = weighted.astype(BF16).astype(F32)
    middle = (weighted - high).astype(BF16).astype(F32)
    low = weighted - high - middle
    combine = jnp.concatenate([high, middle, low], axis=0).astype(BF16)

    for copy in token_copies:
        copy.wait()
    tokens_full = jnp.concatenate(
        [gathered[member].astype(F32) for member in range(n_tp)], axis=1
    )
    h_one = norm_rows(tokens_full, attn_gain[...].reshape(1, -1))

    for name in ("wq", "wk", "wv", "wf"):
        loads[name].wait()
    queries = dot(h_one, wq[...]).astype(BF16).astype(F32)
    key_new = dot_t(h_one, wk[...]).astype(BF16).astype(F32)
    value_new = dot_t(h_one, wv[...]).astype(BF16).astype(F32)
    forget_pre = dot_t(h_one, wf[...]) + forget_bias[...]
    forget_now = jnp.minimum(forget_pre, 0.0) - jnp.log1p(
        jnp.exp(-jnp.abs(forget_pre))
    )
    blank = jnp.zeros((seqs, HD), F32)
    for head in range(heads):
        q3[:, head, :] = jnp.concatenate(
            [queries[:, head * HD : (head + 1) * HD], blank], axis=1
        )
        f3[:, head, :] = jnp.broadcast_to(forget_now[:, head : head + 1], (seqs, 2 * HD))
    kvn[...] = jnp.concatenate([key_new, value_new], axis=1)

    score_scale = HD ** (-0.5)
    position = lax.broadcasted_iota(jnp.int32, (heads, cache_len), 1)
    loads["cum"].wait()

    def attend(seq):
        length = lengths[seq]
        query = q3[seq]
        entries = kv[seq]
        scores = (
            lax.dot_general(
                query.astype(BF16),
                entries,
                (((1,), (1,)), ((), ())),
                preferred_element_type=F32,
            )
            * score_scale
        )
        gates = cum[seq]
        latest = jnp.sum(
            jnp.where(position == length - 1, gates, 0.0), axis=1, keepdims=True
        )
        scores = scores - gates + (latest + f3[seq][:, 0:1])
        scores = jnp.where(position < length, scores, -jnp.inf)
        new_row = kvn[pl.ds(seq, 1), :]
        own_score = jnp.sum(query * new_row, axis=1, keepdims=True) * score_scale
        highest = jnp.maximum(jnp.max(scores, axis=1, keepdims=True), own_score)
        weights = jnp.exp(scores - highest)
        own_weight = jnp.exp(own_score - highest)
        inverse = 1.0 / (jnp.sum(weights, axis=1, keepdims=True) + own_weight)
        blended = dot((weights * inverse).astype(BF16), entries)
        own_weight = (own_weight * inverse).astype(BF16).astype(F32)
        o3[seq] = blended + own_weight * new_row

    for piece in range(kv_parts):
        kv_loads[piece].wait()
        for seq in range(piece * part, (piece + 1) * part):
            attend(seq)
    head_out = jnp.concatenate(
        [o3[:, head, :][:, HD:] for head in range(heads)], axis=1
    ).astype(BF16)

    loads["wo"].wait()
    att_out[...] = dot(head_out, wo[...]).astype(BF16)
    att_copies = [tp_copy(1, step, att_out, att_in.at[step]) for step in range(1, n_tp)]
    for copy in att_copies:
        copy.start()
    attention = att_out[...].astype(F32)
    for step in range(1, n_tp):
        att_copies[step - 1].wait()
        attention = attention + att_in[step].astype(F32)
    residual_full = (tokens_full + attention).astype(BF16)
    h_two = norm_rows(residual_full.astype(F32), ffn_gain[...].reshape(1, -1))
    for member in range(n_tp):
        gathered[member] = residual_full[:, member * width : (member + 1) * width]

    outgoing = dot(either, h_two)
    disp_out[...] = outgoing.reshape(n_ep, cap, n_tp * width).astype(BF16)

    def dispatch(step, carry):
        ep_copy(
            0, step, disp_out.at[lax.rem(me_ep + step, n_ep)], disp_in.at[me_ep]
        ).start()
        return carry

    lax.fori_loop(1, n_ep, dispatch, 0)
    disp_in[me_ep] = disp_out[me_ep]

    for name in ("dg", "du", "dd"):
        loads[name].wait()
    dense_pre = dot(h_two, dg[...])
    dense_act = (dense_pre * jax.nn.sigmoid(dense_pre) * dot(h_two, du[...])).astype(BF16)
    dense_part = dot(dense_act, dd[...]).astype(BF16)
    for member in range(n_tp):
        dense_send[member] = dense_part[:, member * width : (member + 1) * width]
    dense_copies = [
        tp_copy(
            2, step, dense_send.at[lax.rem(me_tp + step, n_tp)], dense_recv.at[step]
        )
        for step in range(1, n_tp)
    ]
    for copy in dense_copies:
        copy.start()
    blend_gate = jax.nn.sigmoid(
        jnp.sum(h_two.astype(F32) * mix_gate[...].reshape(1, -1).astype(F32), axis=1, keepdims=True)
    )

    def dispatched(step, carry):
        ep_copy(
            0, step, disp_out.at[lax.rem(me_ep + step, n_ep)], disp_in.at[me_ep]
        ).wait()
        return carry

    for name in ("eg", "eu", "ed"):
        loads[name].wait()
    lax.fori_loop(1, n_ep, dispatched, 0)

    flat_rows = disp_in[...].astype(F32).reshape(rows, n_tp * width).astype(BF16)
    gate_pre = dot(flat_rows, eg[...])
    hidden = (gate_pre * jax.nn.sigmoid(gate_pre) * dot(flat_rows, eu[...])).astype(BF16)
    exp_copies = []
    for step in list(range(1, n_tp)) + [0]:
        target = lax.rem(me_tp + step, n_tp)
        columns = pl.ds(pl.multiple_of(target * width, width), width)
        exp_send[step] = dot(hidden, ed[:, columns]).astype(BF16)
        if step > 0:
            exp_copies.append(tp_copy(3, step, exp_send.at[step], exp_recv.at[step]))
            exp_copies[-1].start()
    dense_out = dense_send[me_tp].astype(F32)
    for step in range(1, n_tp):
        dense_copies[step - 1].wait()
        dense_out = dense_out + dense_recv[step].astype(F32)
    base = gathered[me_tp].astype(F32) + blend_gate * dense_out
    shares = exp_send[0].astype(F32)
    for step in range(1, n_tp):
        exp_copies[step - 1].wait()
        shares = shares + exp_recv[step].astype(F32)

    ret_out[...] = shares.reshape(n_ep, cap, width).astype(BF16)

    def give_back(step, carry):
        ep_copy(
            1, step, ret_out.at[lax.rem(me_ep + step, n_ep)], ret_in.at[me_ep]
        ).start()
        return carry

    lax.fori_loop(1, n_ep, give_back, 0)
    ret_in[me_ep] = ret_out[me_ep]

    def given_back(step, carry):
        ep_copy(
            1, step, ret_out.at[lax.rem(me_ep + step, n_ep)], ret_in.at[me_ep]
        ).wait()
        return carry

    lax.fori_loop(1, n_ep, given_back, 0)
    returned = ret_in[...].astype(F32).reshape(rows, width).astype(BF16)
    routed = dot(combine, returned)
    routed = routed[:seqs] + routed[seqs : 2 * seqs] + routed[2 * seqs :]
    out[...] = (base + routed).astype(BF16)


def local(
    n_ep,
    n_tp,
    tokens,
    kv_cache,
    cum_gate,
    lengths,
    w_query,
    w_key,
    w_value,
    w_forget,
    forget_bias,
    w_out,
    attn_gain,
    ffn_gain,
    mix_gate,
    expert_gate,
    expert_up,
    expert_down,
    chosen,
    route_weight,
    dense_gate,
    dense_up,
    dense_down,
):
    seqs, width = tokens.shape
    model = n_tp * width
    heads = w_query.shape[1] // HD
    assert w_key.shape[1] == HD
    cap = max(2, (4 * seqs + n_ep - 1) // n_ep)
    cap = (cap + 7) // 8 * 8
    rows = n_ep * cap
    vmem = pl.BlockSpec(memory_space=pltpu.VMEM)
    smem = pl.BlockSpec(memory_space=pltpu.SMEM)
    hbm = pl.BlockSpec(memory_space=pl.ANY)
    like = lambda a: pltpu.VMEM(a.shape, a.dtype)
    return pl.pallas_call(
        functools.partial(kernel, n_ep, n_tp, cap),
        out_shape=jax.ShapeDtypeStruct((seqs, width), BF16),
        in_specs=[vmem, smem] + [vmem] * 6 + [hbm] * 13,
        out_specs=vmem,
        scratch_shapes=[
            like(kv_cache),
            like(cum_gate),
            like(w_query),
            like(w_key.T),
            like(w_value.T),
            like(w_forget.T),
            like(w_out),
            like(expert_gate[0]),
            like(expert_up[0]),
            like(expert_down[0]),
            like(dense_gate),
            like(dense_up),
            like(dense_down),
            pltpu.SemaphoreType.DMA((12,)),
            pltpu.SemaphoreType.DMA((4,)),
            pltpu.VMEM((n_tp, seqs, width), BF16),
            pltpu.VMEM((seqs, heads, 2 * HD), F32),
            pltpu.VMEM((seqs, heads, 2 * HD), F32),
            pltpu.VMEM((seqs, 2 * HD), F32),
            pltpu.VMEM((seqs, heads, 2 * HD), F32),
            pltpu.VMEM((seqs, model), BF16),
            pltpu.VMEM((n_tp, seqs, model), BF16),
            pltpu.VMEM((n_ep, cap, model), BF16),
            pltpu.VMEM((n_ep, cap, model), BF16),
            pltpu.VMEM((n_tp, seqs, width), BF16),
            pltpu.VMEM((n_tp, seqs, width), BF16),
            pltpu.VMEM((n_tp, rows, width), BF16),
            pltpu.VMEM((n_tp, rows, width), BF16),
            pltpu.VMEM((n_ep, cap, width), BF16),
            pltpu.VMEM((n_ep, cap, width), BF16),
            pltpu.SemaphoreType.DMA((4, n_tp)),
            pltpu.SemaphoreType.DMA((4, n_tp)),
            pltpu.SemaphoreType.DMA((2, n_ep)),
            pltpu.SemaphoreType.DMA((2, n_ep)),
        ],
        compiler_params=pltpu.CompilerParams(
            collective_id=0,
            has_side_effects=True,
            vmem_limit_bytes=60 * 1024 * 1024,
        ),
    )(
        tokens,
        lengths,
        forget_bias.reshape(1, -1),
        attn_gain,
        ffn_gain,
        mix_gate,
        chosen.T,
        route_weight.T,
        kv_cache,
        cum_gate,
        w_query,
        w_key.T,
        w_value.T,
        w_forget.T,
        w_out,
        expert_gate,
        expert_up,
        expert_down,
        dense_gate,
        dense_up,
        dense_down,
    )


def solution(mesh):
    in_specs = (
        P("ep", "tp"),
        P("ep", None, "tp"),
        P("ep", "tp", None),
        P("ep"),
        P(None, "tp"),
        P(None, "tp"),
        P(None, "tp"),
        P(None, "tp"),
        P("tp"),
        P("tp", None),
        P(),
        P(),
        P(),
        P("ep", None, "tp"),
        P("ep", None, "tp"),
        P("ep", "tp", None),
        P("ep", None),
        P("ep", None),
        P(None, "tp"),
        P(None, "tp"),
        P("tp", None),
    )
    out_specs = P("ep", "tp")
    return jax.shard_map(
        functools.partial(local, mesh.shape["ep"], mesh.shape["tp"]),
        mesh=mesh,
        in_specs=in_specs,
        out_specs=out_specs,
        check_vma=False,
    )
```

```python
import functools

import jax
import jax.numpy as jnp
from jax import lax
from jax.experimental import pallas as pl
from jax.experimental.pallas import tpu as pltpu
from jax.sharding import PartitionSpec as P

HD = 64
TOP = 2
MESH = pl.DeviceIdType.MESH
F32 = jnp.float32
BF16 = jnp.bfloat16
epsilon = 1e-06


def dot(a, b):
    return jnp.dot(a, b, preferred_element_type=F32)


def dot_t(a, b):
    return lax.dot_general(a, b, (((1,), (1,)), ((), ())), preferred_element_type=F32)


def norm_rows(widened, scales):
    square = jnp.mean(widened * widened, axis=-1, keepdims=True)
    return (widened * lax.rsqrt(square + epsilon) * scales.astype(F32)).astype(BF16)


def kernel(
    n_ep,
    n_tp,
    cap,
    tokens_hbm,
    lengths_hbm,
    forget_bias_hbm,
    attn_gain_hbm,
    ffn_gain_hbm,
    mix_gate_hbm,
    chosen_hbm,
    route_weight_hbm,
    kv_hbm,
    cum_hbm,
    wq_hbm,
    wk_hbm,
    wv_hbm,
    wf_hbm,
    wo_hbm,
    eg_hbm,
    eu_hbm,
    ed_hbm,
    dg_hbm,
    du_hbm,
    dd_hbm,
    out,
    tokens,
    lengths,
    forget_bias,
    attn_gain,
    ffn_gain,
    mix_gate,
    chosen,
    route_weight,
    small_sem,
    kv,
    cum,
    wq,
    wk,
    wv,
    wf,
    wo,
    eg,
    eu,
    ed,
    dg,
    du,
    dd,
    load_sem,
    kv_sem,
    gathered,
    q3,
    f3,
    kvn,
    o3,
    att_out,
    att_in,
    disp_out,
    disp_in,
    dense_send,
    dense_recv,
    exp_send,
    exp_recv,
    ret_out,
    ret_in,
    tp_send,
    tp_recv,
    ep_send,
    ep_recv,
    relay_send,
    relay_recv,
):
    me_tp = lax.axis_index("tp")
    me_ep = lax.axis_index("ep")
    seqs, width = tokens.shape
    heads = cum.shape[1]
    cache_len = kv.shape[1]
    rows = n_ep * cap

    barrier = pltpu.get_barrier_semaphore()
    for step in range(1, n_tp):
        pl.semaphore_signal(
            barrier,
            inc=1,
            device_id={"tp": lax.rem(me_tp + step, n_tp)},
            device_id_type=MESH,
        )

    def greet(step, carry):
        pl.semaphore_signal(
            barrier,
            inc=1,
            device_id={"ep": lax.rem(me_ep + step, n_ep)},
            device_id_type=MESH,
        )
        return carry

    lax.fori_loop(1, n_ep, greet, 0)

    loads = {}

    def load(name, src, dst, sem):
        loads[name] = pltpu.make_async_copy(src, dst, sem)
        loads[name].start()

    load("tokens", tokens_hbm, tokens, small_sem.at[0])
    load("attn_gain", attn_gain_hbm, attn_gain, small_sem.at[1])
    load("chosen", chosen_hbm, chosen, small_sem.at[2])
    load("route_weight", route_weight_hbm, route_weight, small_sem.at[3])
    load("forget_bias", forget_bias_hbm, forget_bias, small_sem.at[4])
    load("lengths", lengths_hbm, lengths, small_sem.at[5])
    load("ffn_gain", ffn_gain_hbm, ffn_gain, small_sem.at[6])
    load("mix_gate", mix_gate_hbm, mix_gate, small_sem.at[7])
    load("wq", wq_hbm, wq, load_sem.at[0])
    load("wk", wk_hbm, wk, load_sem.at[1])
    load("wv", wv_hbm, wv, load_sem.at[2])
    load("wf", wf_hbm, wf, load_sem.at[3])
    load("cum", cum_hbm, cum, load_sem.at[4])
    kv_parts = kv_sem.shape[0]
    part = seqs // kv_parts
    kv_loads = []
    for piece in range(kv_parts):
        span = pl.ds(piece * part, part)
        kv_loads.append(
            pltpu.make_async_copy(kv_hbm.at[span], kv.at[span], kv_sem.at[piece])
        )
        kv_loads[-1].start()

    loads["tokens"].wait()
    pl.semaphore_wait(barrier, n_tp - 1 + n_ep - 1)

    def tp_copy(phase, step, src, dst):
        return pltpu.make_async_remote_copy(
            src_ref=src,
            dst_ref=dst,
            send_sem=tp_send.at[phase, step],
            recv_sem=tp_recv.at[phase, step],
            device_id={"tp": lax.rem(me_tp + step, n_tp)},
            device_id_type=MESH,
        )

    def ep_copy(phase, step, src, dst):
        return pltpu.make_async_remote_copy(
            src_ref=src,
            dst_ref=dst,
            send_sem=ep_send.at[phase, step],
            recv_sem=ep_recv.at[phase, step],
            device_id={"ep": lax.rem(me_ep + step, n_ep)},
            device_id_type=MESH,
        )

    token_copies = [
        tp_copy(0, step, tokens, gathered.at[me_tp]) for step in range(1, n_tp)
    ]
    for copy in token_copies:
        copy.start()
    load("wo", wo_hbm, wo, load_sem.at[5])
    load("dg", dg_hbm, dg, load_sem.at[6])
    load("du", du_hbm, du, load_sem.at[7])
    load("dd", dd_hbm, dd, load_sem.at[8])
    load("eg", eg_hbm.at[0], eg, load_sem.at[9])
    load("eu", eu_hbm.at[0], eu, load_sem.at[10])
    load("ed", ed_hbm.at[0], ed, load_sem.at[11])
    gathered[me_tp] = tokens[...]
    for name in ("attn_gain", "chosen", "route_weight", "forget_bias"):
        loads[name].wait()
    for name in ("lengths", "ffn_gain", "mix_gate"):
        loads[name].wait()

    slot = lax.broadcasted_iota(jnp.int32, (rows, seqs), 0)
    slot_expert = slot // cap
    slot_place = (slot % cap).astype(F32)
    first = (chosen[0:1, :] == slot_expert).astype(F32)
    second = (chosen[1:2, :] == slot_expert).astype(F32)
    either = first + second
    earlier = (
        lax.broadcasted_iota(jnp.int32, (seqs, seqs), 0)
        < lax.broadcasted_iota(jnp.int32, (seqs, seqs), 1)
    ).astype(F32)
    rank = dot(either.astype(BF16), earlier.astype(BF16))
    in_place = (rank == slot_place).astype(F32)
    either = (either * in_place).astype(BF16)
    weighted = first * route_weight[0:1, :] + second * route_weight[1:2, :]
    weighted = jnp.transpose(weighted * in_place)
    high = weighted.astype(BF16).astype(F32)
    middle = (weighted - high).astype(BF16).astype(F32)
    low = weighted - high - middle
    combine = jnp.concatenate([high, middle, low], axis=0).astype(BF16)

    for copy in token_copies:
        copy.wait()
    tokens_full = jnp.concatenate(
        [gathered[member].astype(F32) for member in range(n_tp)], axis=1
    )
    h_one = norm_rows(tokens_full, attn_gain[...].reshape(1, -1))

    for name in ("wq", "wk", "wv", "wf"):
        loads[name].wait()
    queries = dot(h_one, wq[...]).astype(BF16).astype(F32)
    key_new = dot_t(h_one, wk[...]).astype(BF16).astype(F32)
    value_new = dot_t(h_one, wv[...]).astype(BF16).astype(F32)
    forget_pre = dot_t(h_one, wf[...]) + forget_bias[...]
    forget_now = jnp.minimum(forget_pre, 0.0) - jnp.log1p(
        jnp.exp(-jnp.abs(forget_pre))
    )
    blank = jnp.zeros((seqs, HD), F32)
    for head in range(heads):
        q3[:, head, :] = jnp.concatenate(
            [queries[:, head * HD : (head + 1) * HD], blank], axis=1
        )
        f3[:, head, :] = jnp.broadcast_to(forget_now[:, head : head + 1], (seqs, 2 * HD))
    kvn[...] = jnp.concatenate([key_new, value_new], axis=1)

    score_scale = HD ** (-0.5)
    position = lax.broadcasted_iota(jnp.int32, (heads, cache_len), 1)
    loads["cum"].wait()

    def attend(seq):
        length = lengths[seq]
        query = q3[seq]
        entries = kv[seq]
        scores = (
            lax.dot_general(
                query.astype(BF16),
                entries,
                (((1,), (1,)), ((), ())),
                preferred_element_type=F32,
            )
            * score_scale
        )
        gates = cum[seq]
        latest = jnp.sum(
            jnp.where(position == length - 1, gates, 0.0), axis=1, keepdims=True
        )
        scores = scores - gates + (latest + f3[seq][:, 0:1])
        scores = jnp.where(position < length, scores, -jnp.inf)
        new_row = kvn[pl.ds(seq, 1), :]
        own_score = jnp.sum(query * new_row, axis=1, keepdims=True) * score_scale
        highest = jnp.maximum(jnp.max(scores, axis=1, keepdims=True), own_score)
        weights = jnp.exp(scores - highest)
        own_weight = jnp.exp(own_score - highest)
        inverse = 1.0 / (jnp.sum(weights, axis=1, keepdims=True) + own_weight)
        blended = dot((weights * inverse).astype(BF16), entries)
        own_weight = (own_weight * inverse).astype(BF16).astype(F32)
        o3[seq] = blended + own_weight * new_row

    for piece in range(kv_parts):
        kv_loads[piece].wait()
        for seq in range(piece * part, (piece + 1) * part):
            attend(seq)
    head_out = jnp.concatenate(
        [o3[:, head, :][:, HD:] for head in range(heads)], axis=1
    ).astype(BF16)

    loads["wo"].wait()
    att_out[...] = dot(head_out, wo[...]).astype(BF16)
    att_copies = [tp_copy(1, step, att_out, att_in.at[step]) for step in range(1, n_tp)]
    for copy in att_copies:
        copy.start()
    attention = att_out[...].astype(F32)
    for step in range(1, n_tp):
        att_copies[step - 1].wait()
        attention = attention + att_in[step].astype(F32)
    residual_full = (tokens_full + attention).astype(BF16)
    h_two = norm_rows(residual_full.astype(F32), ffn_gain[...].reshape(1, -1))
    for member in range(n_tp):
        gathered[member] = residual_full[:, member * width : (member + 1) * width]

    outgoing = dot(either, h_two)
    half = n_tp * width // 2
    for side in range(2):
        disp_out[side] = (
            outgoing[:, side * half : (side + 1) * half]
            .reshape(n_ep, cap, half)
            .astype(BF16)
        )
    mine = lax.rem(me_tp, 2)
    far_first = sorted(range(1, n_ep), key=lambda step: abs(step - n_ep // 2))
    disp_copies = [
        ep_copy(
            0,
            step,
            disp_out.at[mine, lax.rem(me_ep + step, n_ep)],
            disp_in.at[mine, me_ep],
        )
        for step in far_first
    ]
    for copy in disp_copies:
        copy.start()
    for side in range(2):
        disp_in[side, me_ep] = disp_out[side, me_ep]

    for name in ("dg", "du", "dd"):
        loads[name].wait()
    dense_pre = dot(h_two, dg[...])
    dense_act = (dense_pre * jax.nn.sigmoid(dense_pre) * dot(h_two, du[...])).astype(BF16)
    dense_part = dot(dense_act, dd[...]).astype(BF16)
    for member in range(n_tp):
        dense_send[member] = dense_part[:, member * width : (member + 1) * width]
    dense_copies = [
        tp_copy(
            2, step, dense_send.at[lax.rem(me_tp + step, n_tp)], dense_recv.at[step]
        )
        for step in range(1, n_tp)
    ]
    for copy in dense_copies:
        copy.start()
    blend_gate = jax.nn.sigmoid(
        jnp.sum(h_two.astype(F32) * mix_gate[...].reshape(1, -1).astype(F32), axis=1, keepdims=True)
    )

    relays = []
    for step, copy in reversed(list(zip(far_first, disp_copies))):
        source = lax.rem(me_ep + n_ep - step, n_ep)
        copy.wait_recv()
        relays.append(
            pltpu.make_async_remote_copy(
                src_ref=disp_in.at[mine, source],
                dst_ref=disp_in.at[mine, source],
                send_sem=relay_send.at[step],
                recv_sem=relay_recv.at[step],
                device_id={"tp": me_tp + 1 - 2 * mine},
                device_id_type=MESH,
            )
        )
        relays[-1].start()
    for name in ("eg", "eu", "ed"):
        loads[name].wait()
    for copy in disp_copies:
        copy.wait_send()
    for copy in relays:
        copy.wait()

    flat_rows = jnp.concatenate(
        [disp_in[side].astype(F32).reshape(rows, half) for side in range(2)], axis=1
    ).astype(BF16)
    gate_pre = dot(flat_rows, eg[...])
    hidden = (gate_pre * jax.nn.sigmoid(gate_pre) * dot(flat_rows, eu[...])).astype(BF16)
    exp_copies = []
    for step in list(range(1, n_tp)) + [0]:
        target = lax.rem(me_tp + step, n_tp)
        columns = pl.ds(pl.multiple_of(target * width, width), width)
        exp_send[step] = dot(hidden, ed[:, columns]).astype(BF16)
        if step > 0:
            exp_copies.append(tp_copy(3, step, exp_send.at[step], exp_recv.at[step]))
            exp_copies[-1].start()
    dense_out = dense_send[me_tp].astype(F32)
    for step in range(1, n_tp):
        dense_copies[step - 1].wait()
        dense_out = dense_out + dense_recv[step].astype(F32)
    base = gathered[me_tp].astype(F32) + blend_gate * dense_out
    shares = exp_send[0].astype(F32)
    for step in range(1, n_tp):
        exp_copies[step - 1].wait()
        shares = shares + exp_recv[step].astype(F32)

    ret_out[...] = shares.reshape(n_ep, cap, width).astype(BF16)

    ret_copies = [
        ep_copy(1, step, ret_out.at[lax.rem(me_ep + step, n_ep)], ret_in.at[me_ep])
        for step in far_first
    ]
    for copy in ret_copies:
        copy.start()
    ret_in[me_ep] = ret_out[me_ep]
    for copy in ret_copies:
        copy.wait()
    returned = ret_in[...].astype(F32).reshape(rows, width).astype(BF16)
    routed = dot(combine, returned)
    routed = routed[:seqs] + routed[seqs : 2 * seqs] + routed[2 * seqs :]
    out[...] = (base + routed).astype(BF16)


def local(
    n_ep,
    n_tp,
    tokens,
    kv_cache,
    cum_gate,
    lengths,
    w_query,
    w_key,
    w_value,
    w_forget,
    forget_bias,
    w_out,
    attn_gain,
    ffn_gain,
    mix_gate,
    expert_gate,
    expert_up,
    expert_down,
    chosen,
    route_weight,
    dense_gate,
    dense_up,
    dense_down,
):
    seqs, width = tokens.shape
    model = n_tp * width
    heads = w_query.shape[1] // HD
    assert w_key.shape[1] == HD
    cap = max(2, (4 * seqs + n_ep - 1) // n_ep)
    cap = (cap + 7) // 8 * 8
    rows = n_ep * cap
    vmem = pl.BlockSpec(memory_space=pltpu.VMEM)
    hbm = pl.BlockSpec(memory_space=pl.ANY)
    like = lambda a: pltpu.VMEM(a.shape, a.dtype)
    return pl.pallas_call(
        functools.partial(kernel, n_ep, n_tp, cap),
        out_shape=jax.ShapeDtypeStruct((seqs, width), BF16),
        in_specs=[hbm] * 21,
        out_specs=vmem,
        scratch_shapes=[
            like(tokens),
            pltpu.SMEM(lengths.shape, lengths.dtype),
            pltpu.VMEM((1, heads), F32),
            like(attn_gain),
            like(ffn_gain),
            like(mix_gate),
            like(chosen.T),
            like(route_weight.T),
            pltpu.SemaphoreType.DMA((8,)),
            like(kv_cache),
            like(cum_gate),
            like(w_query),
            like(w_key.T),
            like(w_value.T),
            like(w_forget.T),
            like(w_out),
            like(expert_gate[0]),
            like(expert_up[0]),
            like(expert_down[0]),
            like(dense_gate),
            like(dense_up),
            like(dense_down),
            pltpu.SemaphoreType.DMA((12,)),
            pltpu.SemaphoreType.DMA((4,)),
            pltpu.VMEM((n_tp, seqs, width), BF16),
            pltpu.VMEM((seqs, heads, 2 * HD), F32),
            pltpu.VMEM((seqs, heads, 2 * HD), F32),
            pltpu.VMEM((seqs, 2 * HD), F32),
            pltpu.VMEM((seqs, heads, 2 * HD), F32),
            pltpu.VMEM((seqs, model), BF16),
            pltpu.VMEM((n_tp, seqs, model), BF16),
            pltpu.VMEM((2, n_ep, cap, model // 2), BF16),
            pltpu.VMEM((2, n_ep, cap, model // 2), BF16),
            pltpu.VMEM((n_tp, seqs, width), BF16),
            pltpu.VMEM((n_tp, seqs, width), BF16),
            pltpu.VMEM((n_tp, rows, width), BF16),
            pltpu.VMEM((n_tp, rows, width), BF16),
            pltpu.VMEM((n_ep, cap, width), BF16),
            pltpu.VMEM((n_ep, cap, width), BF16),
            pltpu.SemaphoreType.DMA((4, n_tp)),
            pltpu.SemaphoreType.DMA((4, n_tp)),
            pltpu.SemaphoreType.DMA((2, n_ep)),
            pltpu.SemaphoreType.DMA((2, n_ep)),
            pltpu.SemaphoreType.DMA((n_ep,)),
            pltpu.SemaphoreType.DMA((n_ep,)),
        ],
        compiler_params=pltpu.CompilerParams(
            collective_id=0,
            has_side_effects=True,
            vmem_limit_bytes=60 * 1024 * 1024,
        ),
    )(
        tokens,
        lengths,
        forget_bias.reshape(1, -1),
        attn_gain,
        ffn_gain,
        mix_gate,
        chosen.T,
        route_weight.T,
        kv_cache,
        cum_gate,
        w_query,
        w_key.T,
        w_value.T,
        w_forget.T,
        w_out,
        expert_gate,
        expert_up,
        expert_down,
        dense_gate,
        dense_up,
        dense_down,
    )


def solution(mesh):
    in_specs = (
        P("ep", "tp"),
        P("ep", None, "tp"),
        P("ep", "tp", None),
        P("ep"),
        P(None, "tp"),
        P(None, "tp"),
        P(None, "tp"),
        P(None, "tp"),
        P("tp"),
        P("tp", None),
        P(),
        P(),
        P(),
        P("ep", None, "tp"),
        P("ep", None, "tp"),
        P("ep", "tp", None),
        P("ep", None),
        P("ep", None),
        P(None, "tp"),
        P(None, "tp"),
        P("tp", None),
    )
    out_specs = P("ep", "tp")
    return jax.shard_map(
        functools.partial(local, mesh.shape["ep"], mesh.shape["tp"]),
        mesh=mesh,
        in_specs=in_specs,
        out_specs=out_specs,
        check_vma=False,
    )
```
